1024 devices in a mesh: row: 32 (over z, core), col: 32 (over y, x).
Axes of the slice: x: 4, y: 8, z: 16, core: 2. Of those that a mesh axis runs over, the one named last changes fastest.
Arguments:
- mix_input: bfloat16 [32, 8192, 1024], P('col', 'row'), may hold values from -6 to 6
- gate_logits: bfloat16 [32, 8192, 2048], P('col', 'row'), may hold values from -8 to 8
- w_proj: bfloat16 [1024, 2048], P('col'), may hold values from -0.1875 to 0.1875
Outputs:
- mixed: bfloat16 [32, 8192, 2048], P('col', 'row')
The draws below stay inside these ranges and needn't reach their ends.
All inputs are finite; a program needn't handle non-finite values.
Results may differ from the reference program's by a relative error of at most 0.0049.
Values may be sent and summed in bfloat16 or wider, within the bound.
A program may use at most 32 MiB of HBM per device.

```python
import jax
import jax.numpy as jnp
from jax import lax

D = 2048
GROUP = 256
GROUPS = 4
F = 1024
LENGTH = 8192
SEQS = 32


def steps_of(rng, dims, shards, smallest, top_value):
    factor_of = 1.0
    for axis_at, blocks in shards:
        steps = jax.random.uniform(jax.random.fold_in(jax.random.fold_in(rng, 6), axis_at), (blocks,), jnp.float32, smallest / len(shards), top_value / len(shards))
        factor_of = factor_of * jnp.repeat(jnp.exp(steps), dims[axis_at] // blocks).reshape((-1,) + (1,) * (len(dims) - 1 - axis_at))
    return factor_of


def bell_draw(rng, dims, deviation, reach, shards=(), held_as=jnp.bfloat16):
    entries = jax.random.normal(rng, dims, jnp.float32) * deviation
    if len(shards) > 0:
        entries = steps_of(rng, dims, shards, -0.22, 0.18) * entries
    return jnp.clip(entries, min=-reach, max=reach).astype(held_as)


def setup_inputs(seed: int = 0) -> dict:
    key_list = jax.random.split(jax.random.key(seed), 4)
    return {
        "mix_input": bell_draw(key_list[0], (SEQS, LENGTH, F), 1.0, 6.0, ((0, 32), (1, 32))),
        "gate_logits": bell_draw(key_list[1], (SEQS, LENGTH, D), 1.5, 8.0, ((0, 32), (1, 32))),
        "w_proj": bell_draw(key_list[2], (F, D), F ** -0.5, 0.1875, ((0, 32),)),
    }


def reference(mix_input, gate_logits, w_proj):
    def one_sequence(pair_args):
        signal, logits = pair_args
        grouped = signal.astype(jnp.float32).reshape(LENGTH, GROUPS, GROUP)
        spectrum = jnp.real(jnp.fft.fftn(grouped, axes=(0, 2), norm="ortho")).astype(jnp.float32)
        spectrum_bf = spectrum.reshape(LENGTH, GROUPS * GROUP).astype(jnp.bfloat16)
        projected = jnp.dot(spectrum_bf, w_proj, preferred_element_type=jnp.float32)
        return (jax.nn.sigmoid(logits.astype(jnp.float32)) * projected).astype(jnp.bfloat16)

    return lax.map(one_sequence, (mix_input, gate_logits))
```

```python
import math

import jax
import jax.numpy as jnp
import numpy as np
from jax import lax
from jax.experimental import pallas as pl
from jax.experimental.pallas import tpu as pltpu
from jax.sharding import Mesh
from jax.sharding import PartitionSpec as P

TOKENS = 256
GROUP = 256
LENGTH = 8192
PEERS = 32
ROWS = 16
CHUNKS = 2
Z, CORES, Y, X = 16, 2, 8, 4
HALF = 1024
F32, BF16 = jnp.float32, jnp.bfloat16
BY_MESH = pl.DeviceIdType.MESH
AXES = ("z", "core", "y", "x")


def high_low(table):
    high = table.astype(np.float32).astype(BF16)
    low = (table - high.astype(np.float64)).astype(np.float32).astype(BF16)
    return high, low


def channel_table():
    row = np.arange(GROUP)
    pair = 8 * (row // 16) + row % 8
    imaginary = row // 8 % 2 == 1
    channel = np.arange(GROUP)[None, :]
    angle = 2.0 * np.pi * ((pair[:, None] * channel) % GROUP) / GROUP
    table = np.where(imaginary[:, None], -np.sin(angle), np.cos(angle))
    half_turn = np.where(np.arange(GROUP) % 2 == 0, 1.0, -1.0)
    table[8] = half_turn
    return np.stack(high_low(table))


def position_table():
    t = np.arange(TOKENS)[:, None]
    lane = np.arange(TOKENS)[None, :]
    j = 8 * (lane % 32) + lane // 32
    angle = 2.0 * np.pi * ((t * j) % TOKENS) / TOKENS
    table = np.concatenate([np.cos(angle), np.sin(angle)], 0) / math.sqrt(LENGTH * GROUP)
    return np.stack(high_low(table))


def twist_table():
    angle = 2.0 * np.pi * np.arange(PEERS)[:, None] * np.arange(TOKENS)[None, :] / LENGTH
    return np.stack([np.cos(angle), -np.sin(angle)]).astype(np.float32)


def order_table():
    row = np.arange(GROUP)
    pair = 8 * (row // 16) + row % 8
    upper = row // 8 % 2 == 1
    channel = np.where(upper, np.where(pair == 0, 128, GROUP - pair), pair)
    return (channel[:, None] == np.arange(GROUP)[None, :]).astype(np.float32).astype(BF16)


def times_root(re, im, k, n):
    if k == 0:
        return re, im
    if 4 * k == n:
        return im, -re
    if 8 * k == n:
        h = math.sqrt(0.5)
        return (re + im) * h, (im - re) * h
    if 8 * k == 3 * n:
        h = math.sqrt(0.5)
        return (im - re) * h, (re + im) * -h
    c, s = math.cos(2 * math.pi * k / n), -math.sin(2 * math.pi * k / n)
    return re * c - im * s, re * s + im * c


def fourier(parts):
    n = len(parts)
    if n == 1:
        return parts
    even, odd = fourier(parts[0::2]), fourier(parts[1::2])
    out = [None] * n
    for k in range(n // 2):
        re, im = times_root(*odd[k], k, n)
        out[k] = (even[k][0] + re, even[k][1] + im)
        out[k + n // 2] = (even[k][0] - re, even[k][1] - im)
    return out


def kernel(mix, gate, w_own, chan, posn, twist, order, out, x, gates, chan_v, posn_v, twist_v, order_v, opened,
           w_all, w_ord, send1, recv1, send2, recv2, spec_hi, spec_lo, whole, turned, acc, result,
           load_sem, s1, r1, s2, r2, wx_s, wx_r, plus_s, plus_r, minus_s, minus_r, core_s, core_r, out_sem):
    z, core, y, col = (lax.axis_index(a) for a in AXES)
    me = z * 2 + core
    barrier = pltpu.get_barrier_semaphore()

    def loaded(k, src, dst):
        return pltpu.make_async_copy(src, dst, load_sem.at[k])

    half = pl.ds(pl.multiple_of(core * HALF, HALF), HALF)
    own = y * X + col
    loads = [
        loaded(0, mix.at[0], x),
        loaded(1, chan, chan_v),
        loaded(2, w_own.at[:, half], w_all.at[own, :, half]),
        loaded(3, gate.at[0], gates),
        loaded(4, posn, posn_v),
        loaded(5, twist, twist_v),
        loaded(6, order, order_v),
    ]
    for copy in loads:
        copy.start()

    def greet(d, carry):
        t = lax.rem(me + d, PEERS)
        pl.semaphore_signal(barrier, inc=1, device_id=(t // 2, t % 2, y, col), device_id_type=BY_MESH)
        return carry

    lax.fori_loop(1, PEERS, greet, 0)
    for d in range(1, X):
        pl.semaphore_signal(barrier, inc=1, device_id=(z, core, y, lax.rem(col + d, X)), device_id_type=BY_MESH)
    up, down = lax.rem(y + 1, Y), lax.rem(y + Y - 1, Y)
    for to in (up, down):
        pl.semaphore_signal(barrier, inc=1, device_id=(z, core, to, col), device_id_type=BY_MESH)

    loads[0].wait()
    loads[1].wait()
    for h in range(CHUNKS):
        for g in range(2):
            lanes = pl.ds((2 * h + g) * GROUP, GROUP)
            part = lax.dot_general(chan_v[0], x[:, lanes], (((1,), (1,)), ((), ())), preferred_element_type=F32)
            part = part + lax.dot_general(chan_v[1], x[:, lanes], (((1,), (1,)), ((), ())), preferred_element_type=F32)
            send1[h, pl.ds(16 * g, 16)] = part.astype(BF16).reshape(16, ROWS, TOKENS)
        recv1[h, me] = send1[h, me]
    pl.semaphore_wait(barrier, 31 + 3 + 2)

    def exchange(src, dst, s_sem, r_sem, h):
        def to(tz, tc):
            t = tz * 2 + tc
            pltpu.make_async_remote_copy(
                src.at[h, t], dst.at[h, me], s_sem.at[h], r_sem.at[h], device_id=(tz, tc, y, col), device_id_type=BY_MESH
            ).start()

        def one(i, carry):
            d = 8 - (i + 2) // 4
            k = (i + 2) % 4
            dz = d + (k // 2) * (16 - 2 * d)
            to(lax.rem(z + dz, Z), k % 2)
            return carry

        lax.fori_loop(0, 30, one, 0)
        to(z, 1 - core)

    def landed(buf, sem, h):
        pltpu.make_async_copy(buf.at[h, pl.ds(0, 31)], buf.at[h, pl.ds(0, 31)], sem.at[h]).wait()

    for h in range(CHUNKS):
        exchange(send1, recv1, s1, r1, h)

    loads[2].wait()
    for d in range(1, X):
        pltpu.make_async_remote_copy(
            w_all.at[own, :, half], w_all.at[own, :, half], wx_s, wx_r,
            device_id=(z, core, y, lax.rem(col + d, X)), device_id_type=BY_MESH,
        ).start()

    def block(yb):
        return w_all.at[pl.ds(yb * X, X), :, half]

    def hand_on(yb, to, send, recv):
        pltpu.make_async_remote_copy(
            block(yb), block(yb), send, recv, device_id=(z, core, to, col), device_id_type=BY_MESH
        ).start()

    def to_core(yb, k):
        pltpu.make_async_remote_copy(
            block(yb), block(yb), core_s.at[k], core_r.at[k], device_id=(z, 1 - core, y, col), device_id_type=BY_MESH
        ).start()

    def bytes_of(yb, sem):
        return pltpu.make_async_copy(block(yb), block(yb), sem)

    row3 = w_all.at[pl.ds(0, 3), :, half]
    pltpu.make_async_copy(row3, row3, wx_r).wait()
    hand_on(y, up, plus_s.at[0], plus_r.at[0])
    hand_on(y, down, minus_s.at[0], minus_r.at[0])
    to_core(y, 0)

    def ring(step):
        yb = lax.rem(y + Y - 1 - step, Y)
        bytes_of(yb, plus_r.at[step]).wait()
        if step < 3:
            hand_on(yb, up, plus_s.at[step + 1], plus_r.at[step + 1])
        to_core(yb, 1 + step)
        if step < 3:
            yb = lax.rem(y + 1 + step, Y)
            bytes_of(yb, minus_r.at[step]).wait()
            if step < 2:
                hand_on(yb, down, minus_s.at[step + 1], minus_r.at[step + 1])
            to_core(yb, 5 + step)

    loads[3].wait()

    def open_gate(i, carry):
        rows = pl.ds(pl.multiple_of(i * 16, 16), 16)
        opened[rows, :] = jax.nn.sigmoid(gates[rows, :].astype(F32))
        return carry

    lax.fori_loop(0, TOKENS // 16, open_gate, 0)
    for k in (4, 5, 6):
        loads[k].wait()
    ring(0)

    sub = lax.broadcasted_iota(jnp.int32, (8, 128), 0)
    lane = lax.broadcasted_iota(jnp.int32, (8, 128), 1)
    alone = jnp.logical_and(sub == 0, lax.rem(me, 16) == 0)

    def transform(h):
        def first(i, carry):
            lanes = pl.ds(pl.multiple_of(i * 128, 128), 128)
            lanes_im = pl.ds(pl.multiple_of(i * 128 + TOKENS, 128), 128)
            parts = []
            for r in range(PEERS):
                both = recv1[h, r, :, lanes].astype(F32)
                parts.append((both[:8], both[8:]))
            freq = fourier(parts)
            for k in range(PEERS):
                pr, pi = freq[k]
                mr, mi = freq[(PEERS - k) % PEERS]
                mi = -mi
                lr = jnp.where(alone, (pr + mr) * 0.5, pr)
                li = jnp.where(alone, (pi + mi) * 0.5, pi)
                hr = jnp.where(alone, (pi - mi) * 0.5, mr)
                hi = jnp.where(alone, (mr - pr) * 0.5, mi)
                c = twist_v[0, pl.ds(k, 1), lanes]
                s = twist_v[1, pl.ds(k, 1), lanes]
                re = jnp.concatenate([lr * c - li * s, hr * c - hi * s], 0)
                im = jnp.concatenate([lr * s + li * c, hr * s + hi * c], 0)
                at = pl.ds(k * ROWS, ROWS)
                for val, where in ((re, lanes), (im, lanes_im)):
                    top = val.astype(BF16)
                    spec_hi[at, where] = top
                    spec_lo[at, where] = (val - top.astype(F32)).astype(BF16)
            return carry

        lax.fori_loop(0, 2, first, 0)

        def second(i, carry):
            rows = pl.ds(pl.multiple_of(i * 128, 128), 128)
            top, rest = spec_hi[rows, :], spec_lo[rows, :]
            whole[rows, :] = (
                jnp.dot(top, posn_v[0], preferred_element_type=F32)
                + jnp.dot(rest, posn_v[0], preferred_element_type=F32)
                + jnp.dot(top, posn_v[1], preferred_element_type=F32)
            )
            return carry

        lax.fori_loop(0, 4, second, 0)

        for sign in range(2):
            for part in range(2):
                lanes = pl.ds(part * 128, 128)
                v = [whole[pl.ds(k * ROWS + sign * 8, 8), lanes] for k in range(PEERS)]
                for bit in (1, 2, 4, 8, 16):
                    odd = (lane // bit) % 2 == 1
                    for a in range(PEERS):
                        if a & bit:
                            continue
                        b = a | bit
                        va, vb = v[a], v[b]
                        v[a] = jnp.where(odd, pltpu.roll(vb, bit, 1), va)
                        v[b] = jnp.where(odd, vb, pltpu.roll(va, 128 - bit, 1))
                for r in range(PEERS):
                    turned[r, pl.ds(sign * 8, 8), lanes] = v[r]

        def pack(r, carry):
            send2[h, r] = turned[r].astype(BF16)
            return carry

        lax.fori_loop(0, PEERS, pack, 0)
        recv2[h, me] = send2[h, me]

    landed(recv1, r1, 0)
    transform(0)
    exchange(send2, recv2, s2, r2, 0)
    ring(1)
    ring(2)
    landed(recv1, r1, 1)
    transform(1)
    exchange(send2, recv2, s2, r2, 1)
    ring(3)

    other = pl.ds(pl.multiple_of((1 - core) * HALF, HALF), HALF)
    for k in range(Y):
        theirs = w_all.at[pl.ds(0, X), :, other]
        pltpu.make_async_copy(theirs, theirs, core_r.at[k]).wait()
    for g in range(4):
        def reorder(i, carry):
            lanes = pl.ds(pl.multiple_of(i * 256, 256), 256)
            rows = w_all[pl.ds(g * 8, 8), :, lanes].reshape(GROUP, 256)
            w_ord[pl.ds(g * GROUP, GROUP), lanes] = jnp.dot(order_v[...], rows, preferred_element_type=F32).astype(BF16)
            return carry

        lax.fori_loop(0, 8, reorder, 0)

    landed(recv2, r2, 0)
    spec = recv2[0].reshape(2 * GROUP, TOKENS).T

    def project(i, carry):
        lanes = pl.ds(pl.multiple_of(i * 256, 256), 256)
        acc[:, lanes] = jnp.dot(spec, w_ord[pl.ds(0, 2 * GROUP), lanes], preferred_element_type=F32)
        return carry

    lax.fori_loop(0, 8, project, 0)
    landed(recv2, r2, 1)
    spec_b = recv2[1].reshape(2 * GROUP, TOKENS).T

    def out_copy(i):
        lanes = pl.ds(pl.multiple_of(i * 256, 256), 256)
        return pltpu.make_async_copy(result.at[:, lanes], out.at[0, :, lanes], out_sem.at[i])

    def finish(i, carry):
        lanes = pl.ds(pl.multiple_of(i * 256, 256), 256)
        full = acc[:, lanes] + jnp.dot(spec_b, w_ord[pl.ds(2 * GROUP, 2 * GROUP), lanes], preferred_element_type=F32)
        result[:, lanes] = (opened[:, lanes] * full).astype(BF16)
        out_copy(i).start()
        return carry

    lax.fori_loop(0, 8, finish, 0)

    for h in range(CHUNKS):
        landed(send1, s1, h)
        landed(send2, s2, h)
    pltpu.make_async_copy(row3, row3, wx_s).wait()
    for k in range(4):
        bytes_of(y, plus_s.at[k]).wait()
    for k in range(3):
        bytes_of(y, minus_s.at[k]).wait()
    for k in range(Y):
        bytes_of(y, core_s.at[k]).wait()
    for i in range(8):
        out_copy(i).wait()


def on_device(mix_input, gate_logits, w_proj):
    dma = pltpu.SemaphoreType.DMA
    hbm = pl.BlockSpec(memory_space=pl.ANY)
    vmem = pltpu.VMEM
    return pl.pallas_call(
        kernel,
        out_shape=jax.ShapeDtypeStruct((1, TOKENS, 2048), BF16),
        in_specs=[hbm] * 7,
        out_specs=hbm,
        scratch_shapes=[
            vmem((TOKENS, 1024), BF16),
            vmem((TOKENS, 2048), BF16),
            vmem((2, GROUP, GROUP), BF16),
            vmem((2, 2 * TOKENS, TOKENS), BF16),
            vmem((2, PEERS, TOKENS), F32),
            vmem((GROUP, GROUP), BF16),
            vmem((TOKENS, 2048), F32),
            vmem((32, 32, 2048), BF16),
            vmem((1024, 2048), BF16),
            vmem((CHUNKS, PEERS, ROWS, TOKENS), BF16),
            vmem((CHUNKS, PEERS, ROWS, TOKENS), BF16),
            vmem((CHUNKS, PEERS, ROWS, TOKENS), BF16),
            vmem((CHUNKS, PEERS, ROWS, TOKENS), BF16),
            vmem((PEERS * ROWS, 2 * TOKENS), BF16),
            vmem((PEERS * ROWS, 2 * TOKENS), BF16),
            vmem((PEERS * ROWS, TOKENS), F32),
            vmem((PEERS, ROWS, TOKENS), F32),
            vmem((TOKENS, 2048), F32),
            vmem((TOKENS, 2048), BF16),
            dma((7,)),
            dma((CHUNKS,)), dma((CHUNKS,)), dma((CHUNKS,)), dma((CHUNKS,)),
            dma(()), dma(()),
            dma((4,)), dma((4,)), dma((3,)), dma((3,)),
            dma((Y,)), dma((Y,)),
            dma((8,)),
        ],
        compiler_params=pltpu.CompilerParams(
            collective_id=0, has_side_effects=True, vmem_limit_bytes=60 * 1024 * 1024
        ),
    )(
        mix_input, gate_logits, w_proj,
        jnp.asarray(channel_table()), jnp.asarray(position_table()), jnp.asarray(twist_table()), jnp.asarray(order_table()),
    )


def solution(mesh):
    split = Mesh(mesh.devices.reshape(Z, CORES, Y, X), AXES)
    rows, cols = ("z", "core"), ("y", "x")
    placed = (P(cols, rows, None), P(cols, rows, None), P(cols, None))
    return jax.shard_map(on_device, mesh=split, in_specs=placed, out_specs=P(cols, rows, None), check_vma=False)
```

```python
import math

import jax
import jax.numpy as jnp
import numpy as np
from jax import lax
from jax.experimental import pallas as pl
from jax.experimental.pallas import tpu as pltpu
from jax.sharding import Mesh
from jax.sharding import PartitionSpec as P

TOKENS = 256
GROUP = 256
LENGTH = 8192
PEERS = 32
ROWS = 16
CHUNKS = 2
Z, CORES, Y, X = 16, 2, 8, 4
HALF = 1024
F32, BF16 = jnp.float32, jnp.bfloat16
BY_MESH = pl.DeviceIdType.MESH
AXES = ("z", "core", "y", "x")


def high_low(table):
    high = table.astype(np.float32).astype(BF16)
    low = (table - high.astype(np.float64)).astype(np.float32).astype(BF16)
    return high, low


def channel_table():
    row = np.arange(GROUP)
    pair = 8 * (row // 16) + row % 8
    imaginary = row // 8 % 2 == 1
    channel = np.arange(GROUP)[None, :]
    angle = 2.0 * np.pi * ((pair[:, None] * channel) % GROUP) / GROUP
    table = np.where(imaginary[:, None], -np.sin(angle), np.cos(angle))
    half_turn = np.where(np.arange(GROUP) % 2 == 0, 1.0, -1.0)
    table[8] = half_turn
    return np.stack(high_low(table))


def position_table():
    t = np.arange(TOKENS)[:, None]
    lane = np.arange(TOKENS)[None, :]
    j = 8 * (lane % 32) + lane // 32
    angle = 2.0 * np.pi * ((t * j) % TOKENS) / TOKENS
    table = np.concatenate([np.cos(angle), np.sin(angle)], 0) / math.sqrt(LENGTH * GROUP)
    return np.stack(high_low(table))


def twist_table():
    angle = 2.0 * np.pi * np.arange(PEERS)[:, None] * np.arange(TOKENS)[None, :] / LENGTH
    return np.stack([np.cos(angle), -np.sin(angle)]).astype(np.float32)


def order_table():
    row = np.arange(GROUP)
    pair = 8 * (row // 16) + row % 8
    upper = row // 8 % 2 == 1
    channel = np.where(upper, np.where(pair == 0, 128, GROUP - pair), pair)
    return (channel[:, None] == np.arange(GROUP)[None, :]).astype(np.float32).astype(BF16)


def times_root(re, im, k, n):
    if k == 0:
        return re, im
    if 4 * k == n:
        return im, -re
    if 8 * k == n:
        h = math.sqrt(0.5)
        return (re + im) * h, (im - re) * h
    if 8 * k == 3 * n:
        h = math.sqrt(0.5)
        return (im - re) * h, (re + im) * -h
    c, s = math.cos(2 * math.pi * k / n), -math.sin(2 * math.pi * k / n)
    return re * c - im * s, re * s + im * c


def fourier(parts):
    n = len(parts)
    if n == 1:
        return parts
    even, odd = fourier(parts[0::2]), fourier(parts[1::2])
    out = [None] * n
    for k in range(n // 2):
        re, im = times_root(*odd[k], k, n)
        out[k] = (even[k][0] + re, even[k][1] + im)
        out[k + n // 2] = (even[k][0] - re, even[k][1] - im)
    return out


def kernel(mix, gate, w_own, chan, posn, twist, order, out, x, gates, chan_v, posn_v, twist_v, order_v, opened,
           w_all, w_ord, send1, recv1, send2, recv2, spec_hi, spec_lo, whole, turned, acc,
           load_sem, s1, r1, s2, r2, wx_s, wx_r, plus_s, plus_r, minus_s, minus_r, core_s, core_r):
    z, core, y, col = (lax.axis_index(a) for a in AXES)
    me = z * 2 + core
    barrier = pltpu.get_barrier_semaphore()

    def loaded(k, src, dst):
        return pltpu.make_async_copy(src, dst, load_sem.at[k])

    half = pl.ds(pl.multiple_of(core * HALF, HALF), HALF)
    own = y * X + col
    loads = [
        loaded(0, mix.at[0], x),
        loaded(1, chan, chan_v),
        loaded(2, w_own.at[:, half], w_all.at[own, :, half]),
        loaded(3, gate.at[0], gates),
        loaded(4, posn, posn_v),
        loaded(5, twist, twist_v),
        loaded(6, order, order_v),
    ]
    for copy in loads:
        copy.start()

    def greet(d, carry):
        t = lax.rem(me + d, PEERS)
        pl.semaphore_signal(barrier, inc=1, device_id=(t // 2, t % 2, y, col), device_id_type=BY_MESH)
        return carry

    lax.fori_loop(1, PEERS, greet, 0)
    for d in range(1, X):
        pl.semaphore_signal(barrier, inc=1, device_id=(z, core, y, lax.rem(col + d, X)), device_id_type=BY_MESH)
    up, down = lax.rem(y + 1, Y), lax.rem(y + Y - 1, Y)
    for to in (up, down):
        pl.semaphore_signal(barrier, inc=1, device_id=(z, core, to, col), device_id_type=BY_MESH)

    loads[0].wait()
    loads[1].wait()
    for h in range(CHUNKS):
        for g in range(2):
            lanes = pl.ds((2 * h + g) * GROUP, GROUP)
            part = lax.dot_general(chan_v[0], x[:, lanes], (((1,), (1,)), ((), ())), preferred_element_type=F32)
            part = part + lax.dot_general(chan_v[1], x[:, lanes], (((1,), (1,)), ((), ())), preferred_element_type=F32)
            send1[h, pl.ds(16 * g, 16)] = part.astype(BF16).reshape(16, ROWS, TOKENS)
        recv1[h, me] = send1[h, me]
    pl.semaphore_wait(barrier, 31 + 3 + 2)

    def exchange(src, dst, s_sem, r_sem, h):
        def to(tz, tc):
            t = tz * 2 + tc
            pltpu.make_async_remote_copy(
                src.at[h, t], dst.at[h, me], s_sem.at[h], r_sem.at[h], device_id=(tz, tc, y, col), device_id_type=BY_MESH
            ).start()

        def one(i, carry):
            d = 8 - (i + 2) // 4
            k = (i + 2) % 4
            dz = d + (k // 2) * (16 - 2 * d)
            to(lax.rem(z + dz, Z), k % 2)
            return carry

        lax.fori_loop(0, 30, one, 0)
        to(z, 1 - core)

    def landed(buf, sem, h):
        pltpu.make_async_copy(buf.at[h, pl.ds(0, 31)], buf.at[h, pl.ds(0, 31)], sem.at[h]).wait()

    for h in range(CHUNKS):
        exchange(send1, recv1, s1, r1, h)

    loads[2].wait()
    for d in range(1, X):
        pltpu.make_async_remote_copy(
            w_all.at[own, :, half], w_all.at[own, :, half], wx_s, wx_r,
            device_id=(z, core, y, lax.rem(col + d, X)), device_id_type=BY_MESH,
        ).start()

    def block(yb):
        return w_all.at[pl.ds(yb * X, X), :, half]

    def hand_on(yb, to, send, recv):
        pltpu.make_async_remote_copy(
            block(yb), block(yb), send, recv, device_id=(z, core, to, col), device_id_type=BY_MESH
        ).start()

    def to_core(yb, k):
        pltpu.make_async_remote_copy(
            block(yb), block(yb), core_s.at[k], core_r.at[k], device_id=(z, 1 - core, y, col), device_id_type=BY_MESH
        ).start()

    def bytes_of(yb, sem):
        return pltpu.make_async_copy(block(yb), block(yb), sem)

    row3 = w_all.at[pl.ds(0, 3), :, half]
    pltpu.make_async_copy(row3, row3, wx_r).wait()
    hand_on(y, up, plus_s.at[0], plus_r.at[0])
    hand_on(y, down, minus_s.at[0], minus_r.at[0])
    to_core(y, 0)

    def ring(step):
        yb = lax.rem(y + Y - 1 - step, Y)
        bytes_of(yb, plus_r.at[step]).wait()
        if step < 3:
            hand_on(yb, up, plus_s.at[step + 1], plus_r.at[step + 1])
        to_core(yb, 1 + step)
        if step < 3:
            yb = lax.rem(y + 1 + step, Y)
            bytes_of(yb, minus_r.at[step]).wait()
            if step < 2:
                hand_on(yb, down, minus_s.at[step + 1], minus_r.at[step + 1])
            to_core(yb, 5 + step)

    loads[3].wait()

    def open_gate(i, carry):
        rows = pl.ds(pl.multiple_of(i * 16, 16), 16)
        opened[rows, :] = jax.nn.sigmoid(gates[rows, :].astype(F32))
        return carry

    lax.fori_loop(0, TOKENS // 16, open_gate, 0)
    for k in (4, 5, 6):
        loads[k].wait()
    ring(0)

    sub = lax.broadcasted_iota(jnp.int32, (8, 128), 0)
    lane = lax.broadcasted_iota(jnp.int32, (8, 128), 1)
    alone = jnp.logical_and(sub == 0, lax.rem(me, 16) == 0)

    def transform(h):
        def first(i, carry):
            lanes = pl.ds(pl.multiple_of(i * 128, 128), 128)
            lanes_im = pl.ds(pl.multiple_of(i * 128 + TOKENS, 128), 128)
            parts = []
            for r in range(PEERS):
                both = recv1[h, r, :, lanes].astype(F32)
                parts.append((both[:8], both[8:]))
            freq = fourier(parts)
            for k in range(PEERS):
                pr, pi = freq[k]
                mr, mi = freq[(PEERS - k) % PEERS]
                mi = -mi
                lr = jnp.where(alone, (pr + mr) * 0.5, pr)
                li = jnp.where(alone, (pi + mi) * 0.5, pi)
                hr = jnp.where(alone, (pi - mi) * 0.5, mr)
                hi = jnp.where(alone, (mr - pr) * 0.5, mi)
                c = twist_v[0, pl.ds(k, 1), lanes]
                s = twist_v[1, pl.ds(k, 1), lanes]
                re = jnp.concatenate([lr * c - li * s, hr * c - hi * s], 0)
                im = jnp.concatenate([lr * s + li * c, hr * s + hi * c], 0)
                at = pl.ds(k * ROWS, ROWS)
                for val, where in ((re, lanes), (im, lanes_im)):
                    top = val.astype(BF16)
                    spec_hi[at, where] = top
                    spec_lo[at, where] = (val - top.astype(F32)).astype(BF16)
            return carry

        lax.fori_loop(0, 2, first, 0)

        def second(i, carry):
            rows = pl.ds(pl.multiple_of(i * 128, 128), 128)
            top, rest = spec_hi[rows, :], spec_lo[rows, :]
            whole[rows, :] = (
                jnp.dot(top, posn_v[0], preferred_element_type=F32)
                + jnp.dot(rest, posn_v[0], preferred_element_type=F32)
                + jnp.dot(top, posn_v[1], preferred_element_type=F32)
            )
            return carry

        lax.fori_loop(0, 4, second, 0)

        for sign in range(2):
            for part in range(2):
                lanes = pl.ds(part * 128, 128)
                v = [whole[pl.ds(k * ROWS + sign * 8, 8), lanes] for k in range(PEERS)]
                for bit in (1, 2, 4, 8, 16):
                    odd = (lane // bit) % 2 == 1
                    for a in range(PEERS):
                        if a & bit:
                            continue
                        b = a | bit
                        va, vb = v[a], v[b]
                        v[a] = jnp.where(odd, pltpu.roll(vb, bit, 1), va)
                        v[b] = jnp.where(odd, vb, pltpu.roll(va, 128 - bit, 1))
                for r in range(PEERS):
                    turned[r, pl.ds(sign * 8, 8), lanes] = v[r]

        def pack(r, carry):
            send2[h, r] = turned[r].astype(BF16)
            return carry

        lax.fori_loop(0, PEERS, pack, 0)
        recv2[h, me] = send2[h, me]

    landed(recv1, r1, 0)
    transform(0)
    exchange(send2, recv2, s2, r2, 0)
    ring(1)
    ring(2)
    landed(recv1, r1, 1)
    transform(1)
    exchange(send2, recv2, s2, r2, 1)
    ring(3)

    other = pl.ds(pl.multiple_of((1 - core) * HALF, HALF), HALF)
    for k in range(Y):
        theirs = w_all.at[pl.ds(0, X), :, other]
        pltpu.make_async_copy(theirs, theirs, core_r.at[k]).wait()
    for g in range(4):
        def reorder(i, carry):
            lanes = pl.ds(pl.multiple_of(i * 256, 256), 256)
            rows = w_all[pl.ds(g * 8, 8), :, lanes].reshape(GROUP, 256)
            w_ord[pl.ds(g * GROUP, GROUP), lanes] = jnp.dot(order_v[...], rows, preferred_element_type=F32).astype(BF16)
            return carry

        lax.fori_loop(0, 8, reorder, 0)

    def project(h, rows, final):
        spec = recv2[h, :, :, rows].reshape(2 * GROUP, -1).T
        for i in range(4):
            lanes = pl.ds(i * 512, 512)
            full = jnp.dot(spec, w_ord[pl.ds(h * 2 * GROUP, 2 * GROUP), lanes], preferred_element_type=F32)
            if final:
                out[0, rows, lanes] = (opened[rows, lanes] * (acc[rows, lanes] + full)).astype(BF16)
            else:
                acc[rows, lanes] = full

    landed(recv2, r2, 0)
    project(0, pl.ds(0, TOKENS), False)
    landed(recv2, r2, 1)
    project(1, pl.ds(0, TOKENS), True)

    for h in range(CHUNKS):
        landed(send1, s1, h)
        landed(send2, s2, h)
    pltpu.make_async_copy(row3, row3, wx_s).wait()
    for k in range(4):
        bytes_of(y, plus_s.at[k]).wait()
    for k in range(3):
        bytes_of(y, minus_s.at[k]).wait()
    for k in range(Y):
        bytes_of(y, core_s.at[k]).wait()


def on_device(mix_input, gate_logits, w_proj):
    dma = pltpu.SemaphoreType.DMA
    hbm = pl.BlockSpec(memory_space=pltpu.HBM)
    vmem = pltpu.VMEM
    return pl.pallas_call(
        kernel,
        out_shape=jax.ShapeDtypeStruct((1, TOKENS, 2048), BF16),
        in_specs=[hbm] * 7,
        out_specs=pl.BlockSpec(memory_space=pltpu.VMEM),
        scratch_shapes=[
            vmem((TOKENS, 1024), BF16),
            vmem((TOKENS, 2048), BF16),
            vmem((2, GROUP, GROUP), BF16),
            vmem((2, 2 * TOKENS, TOKENS), BF16),
            vmem((2, PEERS, TOKENS), F32),
            vmem((GROUP, GROUP), BF16),
            vmem((TOKENS, 2048), F32),
            vmem((32, 32, 2048), BF16),
            vmem((1024, 2048), BF16),
            vmem((CHUNKS, PEERS, ROWS, TOKENS), BF16),
            vmem((CHUNKS, PEERS, ROWS, TOKENS), BF16),
            vmem((CHUNKS, PEERS, ROWS, TOKENS), BF16),
            vmem((CHUNKS, PEERS, ROWS, TOKENS), BF16),
            vmem((PEERS * ROWS, 2 * TOKENS), BF16),
            vmem((PEERS * ROWS, 2 * TOKENS), BF16),
            vmem((PEERS * ROWS, TOKENS), F32),
            vmem((PEERS, ROWS, TOKENS), F32),
            vmem((TOKENS, 2048), F32),
            dma((7,)),
            dma((CHUNKS,)), dma((CHUNKS,)), dma((CHUNKS,)), dma((CHUNKS,)),
            dma(()), dma(()),
            dma((4,)), dma((4,)), dma((3,)), dma((3,)),
            dma((Y,)), dma((Y,)),
        ],
        compiler_params=pltpu.CompilerParams(
            collective_id=0, has_side_effects=True, vmem_limit_bytes=28 * 1024 * 1024
        ),
    )(
        *(
            pltpu.with_memory_space_constraint(v, pltpu.HBM)
            for v in (
                mix_input, gate_logits, w_proj,
                jnp.asarray(channel_table()), jnp.asarray(position_table()), jnp.asarray(twist_table()), jnp.asarray(order_table()),
            )
        )
    )


def solution(mesh):
    split = Mesh(mesh.devices.reshape(Z, CORES, Y, X), AXES)
    rows, cols = ("z", "core"), ("y", "x")
    placed = (P(cols, rows, None), P(cols, rows, None), P(cols, None))
    return jax.shard_map(on_device, mesh=split, in_specs=placed, out_specs=P(cols, rows, None), check_vma=False)
```

```python
import math

import jax
import jax.numpy as jnp
import numpy as np
from jax import lax
from jax.experimental import pallas as pl
from jax.experimental.pallas import tpu as pltpu
from jax.sharding import Mesh
from jax.sharding import PartitionSpec as P

TOKENS = 256
GROUP = 256
LENGTH = 8192
PEERS = 32
ROWS = 16
CHUNKS = 2
Z, CORES, Y, X = 16, 2, 8, 4
HALF = 1024
F32, BF16 = jnp.float32, jnp.bfloat16
BY_MESH = pl.DeviceIdType.MESH
AXES = ("z", "core", "y", "x")


def high_low(table):
    high = table.astype(np.float32).astype(BF16)
    low = (table - high.astype(np.float64)).astype(np.float32).astype(BF16)
    return high, low


def channel_table():
    row = np.arange(GROUP)
    pair = 8 * (row // 16) + row % 8
    imaginary = row // 8 % 2 == 1
    channel = np.arange(GROUP)[None, :]
    angle = 2.0 * np.pi * ((pair[:, None] * channel) % GROUP) / GROUP
    table = np.where(imaginary[:, None], -np.sin(angle), np.cos(angle))
    half_turn = np.where(np.arange(GROUP) % 2 == 0, 1.0, -1.0)
    table[8] = half_turn
    return np.stack(high_low(table))


def position_table():
    t = np.arange(TOKENS)[:, None]
    lane = np.arange(TOKENS)[None, :]
    j = 8 * (lane % 32) + lane // 32
    angle = 2.0 * np.pi * ((t * j) % TOKENS) / TOKENS
    table = np.concatenate([np.cos(angle), np.sin(angle)], 0) / math.sqrt(LENGTH * GROUP)
    return np.stack(high_low(table))


def twist_table():
    angle = 2.0 * np.pi * np.arange(PEERS)[:, None] * np.arange(TOKENS)[None, :] / LENGTH
    return np.stack([np.cos(angle), -np.sin(angle)]).astype(np.float32)


def order_table():
    row = np.arange(GROUP)
    pair = 8 * (row // 16) + row % 8
    upper = row // 8 % 2 == 1
    channel = np.where(upper, np.where(pair == 0, 128, GROUP - pair), pair)
    return (channel[:, None] == np.arange(GROUP)[None, :]).astype(np.float32).astype(BF16)


def times_root(re, im, k, n):
    if k == 0:
        return re, im
    if 4 * k == n:
        return im, -re
    if 8 * k == n:
        h = math.sqrt(0.5)
        return (re + im) * h, (im - re) * h
    if 8 * k == 3 * n:
        h = math.sqrt(0.5)
        return (im - re) * h, (re + im) * -h
    c, s = math.cos(2 * math.pi * k / n), -math.sin(2 * math.pi * k / n)
    return re * c - im * s, re * s + im * c


def fourier(parts):
    n = len(parts)
    if n == 1:
        return parts
    even, odd = fourier(parts[0::2]), fourier(parts[1::2])
    out = [None] * n
    for k in range(n // 2):
        re, im = times_root(*odd[k], k, n)
        out[k] = (even[k][0] + re, even[k][1] + im)
        out[k + n // 2] = (even[k][0] - re, even[k][1] - im)
    return out


def kernel(mix, gate, w_own, chan, posn, twist, order, out, x, gates, chan_v, posn_v, twist_v, order_v, opened,
           w_all, w_ord, send1, recv1, send2, recv2, spec_hi, spec_lo, whole, turned, acc,
           load_sem, s1, r1, s2, r2, wx_s, wx_r, plus_s, plus_r, minus_s, minus_r, core_s, core_r):
    z, core, y, col = (lax.axis_index(a) for a in AXES)
    me = z * 2 + core
    barrier = pltpu.get_barrier_semaphore()

    def loaded(k, src, dst):
        return pltpu.make_async_copy(src, dst, load_sem.at[k])

    half = pl.ds(pl.multiple_of(core * HALF, HALF), HALF)
    own = y * X + col
    loads = [
        loaded(0, mix.at[0, :, pl.ds(0, 2 * GROUP)], x.at[:, pl.ds(0, 2 * GROUP)]),
        loaded(1, chan, chan_v),
        loaded(2, w_own.at[:, half], w_all.at[own, :, half]),
        loaded(3, gate.at[0], gates),
        loaded(4, posn, posn_v),
        loaded(5, twist, twist_v),
        loaded(6, order, order_v),
        loaded(7, mix.at[0, :, pl.ds(2 * GROUP, 2 * GROUP)], x.at[:, pl.ds(2 * GROUP, 2 * GROUP)]),
    ]
    for k in (0, 1):
        loads[k].start()

    for d in (8, 7, 9, 6, 10, 5, 11, 4, 12, 3, 13, 2, 14, 1, 15):
        tz = lax.rem(z + d, Z)
        for tc in range(CORES):
            pl.semaphore_signal(barrier, inc=1, device_id=(tz, tc, y, col), device_id_type=BY_MESH)
    pl.semaphore_signal(barrier, inc=1, device_id=(z, 1 - core, y, col), device_id_type=BY_MESH)
    for d in range(1, X):
        pl.semaphore_signal(barrier, inc=1, device_id=(z, core, y, lax.rem(col + d, X)), device_id_type=BY_MESH)
    up, down = lax.rem(y + 1, Y), lax.rem(y + Y - 1, Y)
    for to in (up, down):
        pl.semaphore_signal(barrier, inc=1, device_id=(z, core, to, col), device_id_type=BY_MESH)

    for k in (7, 2, 3, 4, 5, 6):
        loads[k].start()

    def channels(h):
        for g in range(2):
            lanes = pl.ds((2 * h + g) * GROUP, GROUP)
            part = lax.dot_general(chan_v[0], x[:, lanes], (((1,), (1,)), ((), ())), preferred_element_type=F32)
            part = part + lax.dot_general(chan_v[1], x[:, lanes], (((1,), (1,)), ((), ())), preferred_element_type=F32)
            send1[h, pl.ds(16 * g, 16)] = part.astype(BF16).reshape(16, ROWS, TOKENS)
        recv1[h, me] = send1[h, me]

    def exchange(src, dst, s_sem, r_sem, h):
        def to(tz, tc):
            t = tz * 2 + tc
            pltpu.make_async_remote_copy(
                src.at[h, t], dst.at[h, me], s_sem.at[h], r_sem.at[h], device_id=(tz, tc, y, col), device_id_type=BY_MESH
            ).start()

        def one(i, carry):
            d = 8 - (i + 2) // 4
            k = (i + 2) % 4
            dz = d + (k // 2) * (16 - 2 * d)
            to(lax.rem(z + dz, Z), k % 2)
            return carry

        lax.fori_loop(0, 30, one, 0)
        to(z, 1 - core)

    def landed(buf, sem, h):
        pltpu.make_async_copy(buf.at[h, pl.ds(0, 31)], buf.at[h, pl.ds(0, 31)], sem.at[h]).wait()

    loads[0].wait()
    loads[1].wait()
    channels(0)
    pl.semaphore_wait(barrier, 31 + 3 + 2)
    exchange(send1, recv1, s1, r1, 0)
    loads[7].wait()
    channels(1)
    exchange(send1, recv1, s1, r1, 1)

    loads[2].wait()
    for d in range(1, X):
        pltpu.make_async_remote_copy(
            w_all.at[own, :, half], w_all.at[own, :, half], wx_s, wx_r,
            device_id=(z, core, y, lax.rem(col + d, X)), device_id_type=BY_MESH,
        ).start()

    def block(yb):
        return w_all.at[pl.ds(yb * X, X), :, half]

    def hand_on(yb, to, send, recv):
        pltpu.make_async_remote_copy(
            block(yb), block(yb), send, recv, device_id=(z, core, to, col), device_id_type=BY_MESH
        ).start()

    def to_core(yb, k):
        pltpu.make_async_remote_copy(
            block(yb), block(yb), core_s.at[k], core_r.at[k], device_id=(z, 1 - core, y, col), device_id_type=BY_MESH
        ).start()

    def bytes_of(yb, sem):
        return pltpu.make_async_copy(block(yb), block(yb), sem)

    row3 = w_all.at[pl.ds(0, 3), :, half]
    pltpu.make_async_copy(row3, row3, wx_r).wait()
    hand_on(y, up, plus_s.at[0], plus_r.at[0])
    hand_on(y, down, minus_s.at[0], minus_r.at[0])
    to_core(y, 0)

    def ring(step):
        yb = lax.rem(y + Y - 1 - step, Y)
        bytes_of(yb, plus_r.at[step]).wait()
        if step < 3:
            hand_on(yb, up, plus_s.at[step + 1], plus_r.at[step + 1])
        to_core(yb, 1 + step)
        if step < 3:
            yb = lax.rem(y + 1 + step, Y)
            bytes_of(yb, minus_r.at[step]).wait()
            if step < 2:
                hand_on(yb, down, minus_s.at[step + 1], minus_r.at[step + 1])
            to_core(yb, 5 + step)

    loads[3].wait()

    def open_gate(i, carry):
        rows = pl.ds(pl.multiple_of(i * 16, 16), 16)
        opened[rows, :] = jax.nn.sigmoid(gates[rows, :].astype(F32))
        return carry

    lax.fori_loop(0, TOKENS // 16, open_gate, 0)
    for k in (4, 5, 6):
        loads[k].wait()
    ring(0)

    sub = lax.broadcasted_iota(jnp.int32, (8, 128), 0)
    lane = lax.broadcasted_iota(jnp.int32, (8, 128), 1)
    alone = jnp.logical_and(sub == 0, lax.rem(me, 16) == 0)

    def transform(h):
        def first(i, carry):
            lanes = pl.ds(pl.multiple_of(i * 128, 128), 128)
            lanes_im = pl.ds(pl.multiple_of(i * 128 + TOKENS, 128), 128)
            parts = []
            for r in range(PEERS):
                both = recv1[h, r, :, lanes].astype(F32)
                parts.append((both[:8], both[8:]))
            freq = fourier(parts)
            for k in range(PEERS):
                pr, pi = freq[k]
                mr, mi = freq[(PEERS - k) % PEERS]
                mi = -mi
                lr = jnp.where(alone, (pr + mr) * 0.5, pr)
                li = jnp.where(alone, (pi + mi) * 0.5, pi)
                hr = jnp.where(alone, (pi - mi) * 0.5, mr)
                hi = jnp.where(alone, (mr - pr) * 0.5, mi)
                c = twist_v[0, pl.ds(k, 1), lanes]
                s = twist_v[1, pl.ds(k, 1), lanes]
                re = jnp.concatenate([lr * c - li * s, hr * c - hi * s], 0)
                im = jnp.concatenate([lr * s + li * c, hr * s + hi * c], 0)
                at = pl.ds(k * ROWS, ROWS)
                for val, where in ((re, lanes), (im, lanes_im)):
                    top = val.astype(BF16)
                    spec_hi[at, where] = top
                    spec_lo[at, where] = (val - top.astype(F32)).astype(BF16)
            return carry

        lax.fori_loop(0, 2, first, 0)

        def second(i, carry):
            rows = pl.ds(pl.multiple_of(i * 128, 128), 128)
            top, rest = spec_hi[rows, :], spec_lo[rows, :]
            whole[rows, :] = (
                jnp.dot(top, posn_v[0], preferred_element_type=F32)
                + jnp.dot(rest, posn_v[0], preferred_element_type=F32)
                + jnp.dot(top, posn_v[1], preferred_element_type=F32)
            )
            return carry

        lax.fori_loop(0, 4, second, 0)

        for sign in range(2):
            for part in range(2):
                lanes = pl.ds(part * 128, 128)
                v = [whole[pl.ds(k * ROWS + sign * 8, 8), lanes] for k in range(PEERS)]
                for bit in (1, 2, 4, 8, 16):
                    odd = (lane // bit) % 2 == 1
                    for a in range(PEERS):
                        if a & bit:
                            continue
                        b = a | bit
                        va, vb = v[a], v[b]
                        v[a] = jnp.where(odd, pltpu.roll(vb, bit, 1), va)
                        v[b] = jnp.where(odd, vb, pltpu.roll(va, 128 - bit, 1))
                for r in range(PEERS):
                    turned[r, pl.ds(sign * 8, 8), lanes] = v[r]

        def pack(r, carry):
            send2[h, r] = turned[r].astype(BF16)
            return carry

        lax.fori_loop(0, PEERS, pack, 0)
        recv2[h, me] = send2[h, me]

    landed(recv1, r1, 0)
    transform(0)
    exchange(send2, recv2, s2, r2, 0)
    ring(1)
    ring(2)
    landed(recv1, r1, 1)
    transform(1)
    exchange(send2, recv2, s2, r2, 1)
    ring(3)

    other = pl.ds(pl.multiple_of((1 - core) * HALF, HALF), HALF)
    for k in range(Y):
        theirs = w_all.at[pl.ds(0, X), :, other]
        pltpu.make_async_copy(theirs, theirs, core_r.at[k]).wait()
    for g in range(4):
        def reorder(i, carry):
            lanes = pl.ds(pl.multiple_of(i * 256, 256), 256)
            rows = w_all[pl.ds(g * 8, 8), :, lanes].reshape(GROUP, 256)
            w_ord[pl.ds(g * GROUP, GROUP), lanes] = jnp.dot(order_v[...], rows, preferred_element_type=F32).astype(BF16)
            return carry

        lax.fori_loop(0, 8, reorder, 0)

    def project(h, rows, final):
        spec = recv2[h, :, :, rows].reshape(2 * GROUP, -1).T
        for i in range(4):
            lanes = pl.ds(i * 512, 512)
            full = jnp.dot(spec, w_ord[pl.ds(h * 2 * GROUP, 2 * GROUP), lanes], preferred_element_type=F32)
            if final:
                out[0, rows, lanes] = (opened[rows, lanes] * (acc[rows, lanes] + full)).astype(BF16)
            else:
                acc[rows, lanes] = full

    landed(recv2, r2, 0)
    project(0, pl.ds(0, TOKENS), False)
    landed(recv2, r2, 1)
    project(1, pl.ds(0, TOKENS), True)

    for h in range(CHUNKS):
        landed(send1, s1, h)
        landed(send2, s2, h)
    pltpu.make_async_copy(row3, row3, wx_s).wait()
    for k in range(4):
        bytes_of(y, plus_s.at[k]).wait()
    for k in range(3):
        bytes_of(y, minus_s.at[k]).wait()
    for k in range(Y):
        bytes_of(y, core_s.at[k]).wait()


def on_device(mix_input, gate_logits, w_proj):
    dma = pltpu.SemaphoreType.DMA
    hbm = pl.BlockSpec(memory_space=pltpu.HBM)
    vmem = pltpu.VMEM
    return pl.pallas_call(
        kernel,
        out_shape=jax.ShapeDtypeStruct((1, TOKENS, 2048), BF16),
        in_specs=[hbm] * 7,
        out_specs=pl.BlockSpec(memory_space=pltpu.VMEM),
        scratch_shapes=[
            vmem((TOKENS, 1024), BF16),
            vmem((TOKENS, 2048), BF16),
            vmem((2, GROUP, GROUP), BF16),
            vmem((2, 2 * TOKENS, TOKENS), BF16),
            vmem((2, PEERS, TOKENS), F32),
            vmem((GROUP, GROUP), BF16),
            vmem((TOKENS, 2048), F32),
            vmem((32, 32, 2048), BF16),
            vmem((1024, 2048), BF16),
            vmem((CHUNKS, PEERS, ROWS, TOKENS), BF16),
            vmem((CHUNKS, PEERS, ROWS, TOKENS), BF16),
            vmem((CHUNKS, PEERS, ROWS, TOKENS), BF16),
            vmem((CHUNKS, PEERS, ROWS, TOKENS), BF16),
            vmem((PEERS * ROWS, 2 * TOKENS), BF16),
            vmem((PEERS * ROWS, 2 * TOKENS), BF16),
            vmem((PEERS * ROWS, TOKENS), F32),
            vmem((PEERS, ROWS, TOKENS), F32),
            vmem((TOKENS, 2048), F32),
            dma((8,)),
            dma((CHUNKS,)), dma((CHUNKS,)), dma((CHUNKS,)), dma((CHUNKS,)),
            dma(()), dma(()),
            dma((4,)), dma((4,)), dma((3,)), dma((3,)),
            dma((Y,)), dma((Y,)),
        ],
        compiler_params=pltpu.CompilerParams(
            collective_id=0, has_side_effects=True, vmem_limit_bytes=28 * 1024 * 1024
        ),
    )(
        *(
            pltpu.with_memory_space_constraint(v, pltpu.HBM)
            for v in (
                mix_input, gate_logits, w_proj,
                jnp.asarray(channel_table()), jnp.asarray(position_table()), jnp.asarray(twist_table()), jnp.asarray(order_table()),
            )
        )
    )


def solution(mesh):
    split = Mesh(mesh.devices.reshape(Z, CORES, Y, X), AXES)
    rows, cols = ("z", "core"), ("y", "x")
    placed = (P(cols, rows, None), P(cols, rows, None), P(cols, None))
    return jax.shard_map(on_device, mesh=split, in_specs=placed, out_specs=P(cols, rows, None), check_vma=False)
```

```python
import math

import jax
import jax.numpy as jnp
import numpy as np
from jax import lax
from jax.experimental import pallas as pl
from jax.experimental.pallas import tpu as pltpu
from jax.sharding import Mesh
from jax.sharding import PartitionSpec as P

TOKENS = 256
GROUP = 256
LENGTH = 8192
PEERS = 32
ROWS = 16
CHUNKS = 2
Z, CORES, Y, X = 16, 2, 8, 4
HALF = 1024
F32, BF16 = jnp.float32, jnp.bfloat16
BY_MESH = pl.DeviceIdType.MESH
AXES = ("z", "core", "y", "x")


def high_low(table):
    high = table.astype(np.float32).astype(BF16)
    low = (table - high.astype(np.float64)).astype(np.float32).astype(BF16)
    return high, low


def channel_table():
    row = np.arange(GROUP)
    pair = 8 * (row // 16) + row % 8
    imaginary = row // 8 % 2 == 1
    channel = np.arange(GROUP)[None, :]
    angle = 2.0 * np.pi * ((pair[:, None] * channel) % GROUP) / GROUP
    table = np.where(imaginary[:, None], -np.sin(angle), np.cos(angle))
    half_turn = np.where(np.arange(GROUP) % 2 == 0, 1.0, -1.0)
    table[8] = half_turn
    return np.stack(high_low(table))


def position_table():
    t = np.arange(TOKENS)[:, None]
    lane = np.arange(TOKENS)[None, :]
    j = 8 * (lane % 32) + lane // 32
    angle = 2.0 * np.pi * ((t * j) % TOKENS) / TOKENS
    table = np.concatenate([np.cos(angle), np.sin(angle)], 0) / math.sqrt(LENGTH * GROUP)
    return np.stack(high_low(table))


def twist_table():
    angle = 2.0 * np.pi * np.arange(PEERS)[:, None] * np.arange(TOKENS)[None, :] / LENGTH
    return np.stack([np.cos(angle), -np.sin(angle)]).astype(np.float32)


def order_table():
    row = np.arange(GROUP)
    pair = 8 * (row // 16) + row % 8
    upper = row // 8 % 2 == 1
    channel = np.where(upper, np.where(pair == 0, 128, GROUP - pair), pair)
    return (channel[:, None] == np.arange(GROUP)[None, :]).astype(np.float32).astype(BF16)


def times_root(re, im, k, n):
    if k == 0:
        return re, im
    if 4 * k == n:
        return im, -re
    if 8 * k == n:
        h = math.sqrt(0.5)
        return (re + im) * h, (im - re) * h
    if 8 * k == 3 * n:
        h = math.sqrt(0.5)
        return (im - re) * h, (re + im) * -h
    c, s = math.cos(2 * math.pi * k / n), -math.sin(2 * math.pi * k / n)
    return re * c - im * s, re * s + im * c


def fourier(parts):
    n = len(parts)
    if n == 1:
        return parts
    even, odd = fourier(parts[0::2]), fourier(parts[1::2])
    out = [None] * n
    for k in range(n // 2):
        re, im = times_root(*odd[k], k, n)
        out[k] = (even[k][0] + re, even[k][1] + im)
        out[k + n // 2] = (even[k][0] - re, even[k][1] - im)
    return out


def kernel(mix, gate, w_own, chan, posn, twist, order, out, x, gates, chan_v, posn_v, twist_v, order_v, opened,
           w_all, w_ord, send1, recv1, send2, recv2, spec_hi, spec_lo, whole, turned, acc,
           load_sem, s1, r1, s2, r2, wx_s, wx_r, plus_s, plus_r, minus_s, minus_r, core_s, core_r):
    z, core, y, col = (lax.axis_index(a) for a in AXES)
    me = z * 2 + core
    barrier = pltpu.get_barrier_semaphore()

    def loaded(k, src, dst):
        return pltpu.make_async_copy(src, dst, load_sem.at[k])

    half = pl.ds(pl.multiple_of(core * HALF, HALF), HALF)
    own = y * X + col
    loads = [
        loaded(0, mix.at[0, :, pl.ds(0, 2 * GROUP)], x.at[:, pl.ds(0, 2 * GROUP)]),
        loaded(1, chan, chan_v),
        loaded(2, w_own.at[:, half], w_all.at[own, :, half]),
        loaded(3, gate.at[0], gates),
        loaded(4, posn, posn_v),
        loaded(5, twist, twist_v),
        loaded(6, order, order_v),
        loaded(7, mix.at[0, :, pl.ds(2 * GROUP, 2 * GROUP)], x.at[:, pl.ds(2 * GROUP, 2 * GROUP)]),
    ]
    for k in (0, 1):
        loads[k].start()

    for d in (8, 7, 9, 6, 10, 5, 11, 4, 12, 3, 13, 2, 14, 1, 15):
        tz = lax.rem(z + d, Z)
        for tc in range(CORES):
            pl.semaphore_signal(barrier, inc=1, device_id=(tz, tc, y, col), device_id_type=BY_MESH)
    pl.semaphore_signal(barrier, inc=1, device_id=(z, 1 - core, y, col), device_id_type=BY_MESH)
    for d in range(1, X):
        pl.semaphore_signal(barrier, inc=1, device_id=(z, core, y, lax.rem(col + d, X)), device_id_type=BY_MESH)
    up, down = lax.rem(y + 1, Y), lax.rem(y + Y - 1, Y)
    for to in (up, down):
        pl.semaphore_signal(barrier, inc=1, device_id=(z, core, to, col), device_id_type=BY_MESH)

    for k in (7, 2, 3, 4, 5, 6):
        loads[k].start()

    def channels(h):
        for g in range(2):
            lanes = pl.ds((2 * h + g) * GROUP, GROUP)
            part = lax.dot_general(chan_v[0], x[:, lanes], (((1,), (1,)), ((), ())), preferred_element_type=F32)
            part = part + lax.dot_general(chan_v[1], x[:, lanes], (((1,), (1,)), ((), ())), preferred_element_type=F32)
            send1[h, pl.ds(16 * g, 16)] = part.astype(BF16).reshape(16, ROWS, TOKENS)
        recv1[h, me] = send1[h, me]

    def exchange(src, dst, s_sem, r_sem, h):
        def to(tz, tc):
            t = tz * 2 + tc
            pltpu.make_async_remote_copy(
                src.at[h, t], dst.at[h, me], s_sem.at[h], r_sem.at[h], device_id=(tz, tc, y, col), device_id_type=BY_MESH
            ).start()

        def one(i, carry):
            d = 8 - (i + 2) // 4
            k = (i + 2) % 4
            dz = d + (k // 2) * (16 - 2 * d)
            to(lax.rem(z + dz, Z), k % 2)
            return carry

        lax.fori_loop(0, 30, one, 0)
        to(z, 1 - core)

    def landed(buf, sem, h):
        pltpu.make_async_copy(buf.at[h, pl.ds(0, 31)], buf.at[h, pl.ds(0, 31)], sem.at[h]).wait()

    loads[0].wait()
    loads[1].wait()
    channels(0)
    pl.semaphore_wait(barrier, 31 + 3 + 2)
    exchange(send1, recv1, s1, r1, 0)
    loads[7].wait()
    channels(1)
    exchange(send1, recv1, s1, r1, 1)

    loads[2].wait()
    for d in range(1, X):
        pltpu.make_async_remote_copy(
            w_all.at[own, :, half], w_all.at[own, :, half], wx_s, wx_r,
            device_id=(z, core, y, lax.rem(col + d, X)), device_id_type=BY_MESH,
        ).start()

    def block(yb):
        return w_all.at[pl.ds(yb * X, X), :, half]

    def hand_on(yb, to, send, recv):
        pltpu.make_async_remote_copy(
            block(yb), block(yb), send, recv, device_id=(z, core, to, col), device_id_type=BY_MESH
        ).start()

    def to_core(yb, k):
        pltpu.make_async_remote_copy(
            block(yb), block(yb), core_s.at[k], core_r.at[k], device_id=(z, 1 - core, y, col), device_id_type=BY_MESH
        ).start()

    def bytes_of(yb, sem):
        return pltpu.make_async_copy(block(yb), block(yb), sem)

    row3 = w_all.at[pl.ds(0, 3), :, half]
    pltpu.make_async_copy(row3, row3, wx_r).wait()
    hand_on(y, up, plus_s.at[0], plus_r.at[0])
    hand_on(y, down, minus_s.at[0], minus_r.at[0])
    to_core(y, 0)

    def ring(step):
        yb = lax.rem(y + Y - 1 - step, Y)
        bytes_of(yb, plus_r.at[step]).wait()
        if step < 3:
            hand_on(yb, up, plus_s.at[step + 1], plus_r.at[step + 1])
        to_core(yb, 1 + step)
        if step < 3:
            yb = lax.rem(y + 1 + step, Y)
            bytes_of(yb, minus_r.at[step]).wait()
            if step < 2:
                hand_on(yb, down, minus_s.at[step + 1], minus_r.at[step + 1])
            to_core(yb, 5 + step)

    loads[3].wait()

    def open_gate(i, carry):
        rows = pl.ds(pl.multiple_of(i * 16, 16), 16)
        opened[rows, :] = jax.nn.sigmoid(gates[rows, :].astype(F32))
        return carry

    lax.fori_loop(0, TOKENS // 16, open_gate, 0)
    for k in (4, 5, 6):
        loads[k].wait()
    ring(0)

    sub = lax.broadcasted_iota(jnp.int32, (8, 128), 0)
    lane = lax.broadcasted_iota(jnp.int32, (8, 128), 1)
    alone = jnp.logical_and(sub == 0, lax.rem(me, 16) == 0)

    def transform(h):
        def first(i, carry):
            lanes = pl.ds(pl.multiple_of(i * 128, 128), 128)
            lanes_im = pl.ds(pl.multiple_of(i * 128 + TOKENS, 128), 128)
            parts = []
            for r in range(PEERS):
                both = recv1[h, r, :, lanes].astype(F32)
                parts.append((both[:8], both[8:]))
            freq = fourier(parts)
            for k in range(PEERS):
                pr, pi = freq[k]
                mr, mi = freq[(PEERS - k) % PEERS]
                mi = -mi
                lr = jnp.where(alone, (pr + mr) * 0.5, pr)
                li = jnp.where(alone, (pi + mi) * 0.5, pi)
                hr = jnp.where(alone, (pi - mi) * 0.5, mr)
                hi = jnp.where(alone, (mr - pr) * 0.5, mi)
                c = twist_v[0, pl.ds(k, 1), lanes]
                s = twist_v[1, pl.ds(k, 1), lanes]
                re = jnp.concatenate([lr * c - li * s, hr * c - hi * s], 0)
                im = jnp.concatenate([lr * s + li * c, hr * s + hi * c], 0)
                at = pl.ds(k * ROWS, ROWS)
                for val, where in ((re, lanes), (im, lanes_im)):
                    top = val.astype(BF16)
                    spec_hi[at, where] = top
                    spec_lo[at, where] = (val - top.astype(F32)).astype(BF16)
            return carry

        lax.fori_loop(0, 2, first, 0)

        def second(i, carry):
            rows = pl.ds(pl.multiple_of(i * 128, 128), 128)
            top, rest = spec_hi[rows, :], spec_lo[rows, :]
            whole[rows, :] = (
                jnp.dot(top, posn_v[0], preferred_element_type=F32)
                + jnp.dot(rest, posn_v[0], preferred_element_type=F32)
                + jnp.dot(top, posn_v[1], preferred_element_type=F32)
            )
            return carry

        lax.fori_loop(0, 4, second, 0)

        for sign in range(2):
            for part in range(2):
                lanes = pl.ds(part * 128, 128)
                v = [whole[pl.ds(k * ROWS + sign * 8, 8), lanes] for k in range(PEERS)]
                for bit in (1, 2, 4, 8, 16):
                    odd = (lane // bit) % 2 == 1
                    for a in range(PEERS):
                        if a & bit:
                            continue
                        b = a | bit
                        va, vb = v[a], v[b]
                        v[a] = jnp.where(odd, pltpu.roll(vb, bit, 1), va)
                        v[b] = jnp.where(odd, vb, pltpu.roll(va, 128 - bit, 1))
                for r in range(PEERS):
                    turned[r, pl.ds(sign * 8, 8), lanes] = v[r]

        def pack(r, carry):
            send2[h, r] = turned[r].astype(BF16)
            return carry

        lax.fori_loop(0, PEERS, pack, 0)
        recv2[h, me] = send2[h, me]

    landed(recv1, r1, 0)
    transform(0)
    exchange(send2, recv2, s2, r2, 0)
    ring(1)
    ring(2)
    landed(recv1, r1, 1)
    transform(1)
    exchange(send2, recv2, s2, r2, 1)
    ring(3)

    other = pl.ds(pl.multiple_of((1 - core) * HALF, HALF), HALF)
    for k in range(Y):
        theirs = w_all.at[pl.ds(0, X), :, other]
        pltpu.make_async_copy(theirs, theirs, core_r.at[k]).wait()
    for g in range(4):
        def reorder(i, carry):
            lanes = pl.ds(pl.multiple_of(i * 256, 256), 256)
            rows = w_all[pl.ds(g * 8, 8), :, lanes].reshape(GROUP, 256)
            w_ord[pl.ds(g * GROUP, GROUP), lanes] = jnp.dot(order_v[...], rows, preferred_element_type=F32).astype(BF16)
            return carry

        lax.fori_loop(0, 8, reorder, 0)

    def project(h, rows, final):
        spec = recv2[h, :, :, rows].reshape(2 * GROUP, -1).T
        for i in range(2):
            lanes = pl.ds(i * 1024, 1024)
            full = jnp.dot(spec, w_ord[pl.ds(h * 2 * GROUP, 2 * GROUP), lanes], preferred_element_type=F32)
            if final:
                out[0, rows, lanes] = (opened[rows, lanes] * (acc[rows, lanes] + full)).astype(BF16)
            else:
                acc[rows, lanes] = full

    landed(recv2, r2, 0)
    project(0, pl.ds(0, TOKENS), False)
    landed(recv2, r2, 1)
    project(1, pl.ds(0, TOKENS), True)

    for h in range(CHUNKS):
        landed(send1, s1, h)
        landed(send2, s2, h)
    pltpu.make_async_copy(row3, row3, wx_s).wait()
    for k in range(4):
        bytes_of(y, plus_s.at[k]).wait()
    for k in range(3):
        bytes_of(y, minus_s.at[k]).wait()
    for k in range(Y):
        bytes_of(y, core_s.at[k]).wait()


def on_device(mix_input, gate_logits, w_proj):
    dma = pltpu.SemaphoreType.DMA
    hbm = pl.BlockSpec(memory_space=pltpu.HBM)
    vmem = pltpu.VMEM
    return pl.pallas_call(
        kernel,
        out_shape=jax.ShapeDtypeStruct((1, TOKENS, 2048), BF16),
        in_specs=[hbm] * 7,
        out_specs=pl.BlockSpec(memory_space=pltpu.VMEM),
        scratch_shapes=[
            vmem((TOKENS, 1024), BF16),
            vmem((TOKENS, 2048), BF16),
            vmem((2, GROUP, GROUP), BF16),
            vmem((2, 2 * TOKENS, TOKENS), BF16),
            vmem((2, PEERS, TOKENS), F32),
            vmem((GROUP, GROUP), BF16),
            vmem((TOKENS, 2048), F32),
            vmem((32, 32, 2048), BF16),
            vmem((1024, 2048), BF16),
            vmem((CHUNKS, PEERS, ROWS, TOKENS), BF16),
            vmem((CHUNKS, PEERS, ROWS, TOKENS), BF16),
            vmem((CHUNKS, PEERS, ROWS, TOKENS), BF16),
            vmem((CHUNKS, PEERS, ROWS, TOKENS), BF16),
            vmem((PEERS * ROWS, 2 * TOKENS), BF16),
            vmem((PEERS * ROWS, 2 * TOKENS), BF16),
            vmem((PEERS * ROWS, TOKENS), F32),
            vmem((PEERS, ROWS, TOKENS), F32),
            vmem((TOKENS, 2048), F32),
            dma((8,)),
            dma((CHUNKS,)), dma((CHUNKS,)), dma((CHUNKS,)), dma((CHUNKS,)),
            dma(()), dma(()),
            dma((4,)), dma((4,)), dma((3,)), dma((3,)),
            dma((Y,)), dma((Y,)),
        ],
        compiler_params=pltpu.CompilerParams(
            collective_id=0, has_side_effects=True, vmem_limit_bytes=28 * 1024 * 1024
        ),
    )(
        *(
            pltpu.with_memory_space_constraint(v, pltpu.HBM)
            for v in (
                mix_input, gate_logits, w_proj,
                jnp.asarray(channel_table()), jnp.asarray(position_table()), jnp.asarray(twist_table()), jnp.asarray(order_table()),
            )
        )
    )


def solution(mesh):
    split = Mesh(mesh.devices.reshape(Z, CORES, Y, X), AXES)
    rows, cols = ("z", "core"), ("y", "x")
    placed = (P(cols, rows, None), P(cols, rows, None), P(cols, None))
    return jax.shard_map(on_device, mesh=split, in_specs=placed, out_specs=P(cols, rows, None), check_vma=False)
```
